32 devices in a mesh: ep: 8 (over z, y), tp: 4 (over x, core).
Axes of the slice: x: 2, y: 2, z: 4, core: 2. Of those that a mesh axis runs over, the one named last changes fastest.
Arguments:
- tokens: bfloat16 [1024, 2048], P('ep'), may hold values from -6 to 6
- norm_gain: float32 [2048], replicated, may hold values from 0.1 to 1.9
- expert_ids: int32 [1024, 6], P('ep'), may hold values from 0 to 15, all different within a row; in each aligned block of 128 rows (0 to 127, 128 to 255, ...) at most 96 rows name the same one
- route_weights: float32 [1024, 6], P('ep'), may hold values from 0.1 to 1
- expert_gate: bfloat16 [32, 2048, 256], P(('ep', 'tp')), may hold values from -0.125 to 0.125
- expert_up: bfloat16 [32, 2048, 256], P(('ep', 'tp')), may hold values from -0.125 to 0.125
- expert_down: bfloat16 [32, 256, 2048], P(('ep', 'tp')), may hold values from -0.25 to 0.25
- shared_gate: bfloat16 [2048, 512], P(None, 'tp'), may hold values from -0.125 to 0.125
- shared_up: bfloat16 [2048, 512], P(None, 'tp'), may hold values from -0.125 to 0.125
- shared_down: bfloat16 [512, 2048], P(None, 'tp'), may hold values from -0.25 to 0.25
Outputs:
- mixed: bfloat16 [1024, 2048], P('ep', 'tp')
The draws below stay inside these ranges and needn't reach their ends.
Inputs may be any that keep to these rules, and one draw needn't show every extreme that they name: `expert_ids`: each row names 6 different experts. In each aligned block of 128 rows (the rows of one index of ep) no expert is named by more than 96 rows, a bound that some block reaches.
All inputs are finite; a program needn't handle non-finite values.
Results may differ from the reference program's by a relative error of at most 0.0073.
Values may be sent and summed in bfloat16 or wider, within the bound.
A program may use at most 64 MiB of HBM per device.

```python
import math
import jax
import jax.numpy as jnp
import numpy as np
from jax import lax

D = 2048
EXPERT_FF = 512
SHARED_FF = 512
TOP_K = 6
TOK_DEV = 128
EXP_HALF = 256
EXPERTS = 16
CAP = 96
TOKENS = 1024
N_EP = 8


def level_of(stream_key, extent, split, low, high):
    def one(dim, shards_of):
        heights = jax.random.uniform(jax.random.fold_in(jax.random.fold_in(stream_key, 6), dim), (shards_of,), jnp.float32, low / len(split), high / len(split))
        return jnp.repeat(jnp.exp(heights), extent[dim] // shards_of).reshape((-1,) + (1,) * (len(extent) - dim - 1))

    loudness = one(*split[0])
    for cut in split[1:]:
        loudness = loudness * one(*cut)
    return loudness


def deal_out(rng, own, number, rows, amount, top, bound, slope):
    ranking = jax.random.permutation(rng, amount)
    crowded, usual = portions_of(amount, rows * top, bound, slope, True), portions_of(amount, rows * top, bound, slope, False)
    places = jnp.arange(amount)

    def named(tallies, turn):
        used = int((tallies > 0).sum())
        fixed = max(1, used // 4)
        passed = fixed + (places - fixed + turn * (used - fixed)) % max(1, amount - fixed)
        return jnp.zeros((amount,), jnp.int32).at[ranking[jnp.where(places < fixed, places, passed)]].set(jnp.asarray(tallies, jnp.int32))

    tallies = jnp.where(number % 4 == 0, named(crowded, number // 4), named(usual, number - number // 4 - 1))
    mixed = jax.random.permutation(jax.random.fold_in(own, 3), amount)
    donor, taker = mixed[0:amount // 2 * 2:2], mixed[1:amount // 2 * 2:2]
    room = jnp.minimum(tallies[donor] - 1, bound - tallies[taker]) // 2
    room = jnp.where((donor == ranking[0]) | (taker == ranking[0]) | (tallies[taker] == 0), 0, jnp.maximum(room, 0))
    passed = jax.random.randint(jax.random.fold_in(own, 4), (amount // 2,), 0, 1 << 20) % (room + 1)
    tallies = tallies.at[donor].add(-passed).at[taker].add(passed)
    labels = jnp.searchsorted(jnp.cumsum(tallies), jnp.arange(rows * top), side="right").astype(jnp.int32)
    listing = labels.reshape(top, rows).T
    listing = listing[jax.random.permutation(jax.random.fold_in(own, 1), rows)]
    turn = jax.random.randint(jax.random.fold_in(own, 2), (rows, 1), 0, top)
    return jnp.take_along_axis(listing, (jnp.arange(top)[None, :] + turn) % top, axis=1)


def portions_of(count, total, reach, slope, full):
    loads = [(1 << 20) // math.isqrt(grade ** slope) + 1 for grade in range(1, count + 1)]
    largest = reach if full else min(reach, max(-(-total // count), total * loads[0] // sum(loads)))
    least = 1 if total - largest >= count - 1 else 0
    given, spare = [largest] + [least] * (count - 1), total - largest - least * (count - 1)
    while spare > 0:
        movable = [i for i in range(1, count) if given[i] < largest] or [i for i in range(1, count) if given[i] < reach]
        mass, budget = sum([loads[i] for i in movable]), spare
        for i in movable:
            addition = min(reach - given[i], max(1, budget * loads[i] // mass), spare)
            given[i] = given[i] + addition
            spare = spare - addition
    return np.array(given)


def bell_draw(stream_key, extent, spread, most, cuts=(), held_as=jnp.bfloat16):
    array = spread * jax.random.normal(stream_key, extent, jnp.float32)
    if cuts:
        array = array * level_of(stream_key, extent, cuts, -0.22, 0.18)
    return jnp.clip(array, -most, most).astype(held_as)


def setup_inputs(seed: int = 0) -> dict:
    keys = jax.random.split(jax.random.key(seed), 11)
    tokens = bell_draw(keys[0], (TOKENS, D), 1.0, 6.0, ((0, 8),))
    norm_gain = jnp.clip(1.0 + 0.18 * jax.random.normal(keys[1], (D,), jnp.float32), 0.1, 1.9)
    expert_ids_keys = jax.random.split(jax.random.fold_in(keys[2], 1), TOKENS // TOK_DEV)
    expert_ids_turns = jax.random.permutation(jax.random.fold_in(keys[2], 3), TOKENS // TOK_DEV)
    expert_ids = jax.vmap(lambda own, number: deal_out(jax.random.fold_in(keys[2], 2), own, number, TOK_DEV, EXPERTS, TOP_K, CAP, 2))(expert_ids_keys, expert_ids_turns).reshape((TOKENS, TOP_K))
    route_weights = jnp.clip(jnp.exp(math.log(1.0) - 2.3025851 * jax.random.uniform(keys[3], (TOKENS, TOP_K), jnp.float32) ** level_of(keys[3], (TOKENS, TOP_K), ((0, 8),), -0.2, 0.2)), 0.1, 1.0)
    expert_gate = bell_draw(keys[4], (2 * EXPERTS, D, EXP_HALF), D ** -0.5, 0.125, ((0, 32),))
    expert_up = bell_draw(keys[5], (2 * EXPERTS, D, EXP_HALF), D ** -0.5, 0.125, ((0, 32),))
    expert_down = bell_draw(keys[6], (2 * EXPERTS, EXP_HALF, D), EXPERT_FF ** -0.5, 0.25, ((0, 32),))
    shared_gate = bell_draw(keys[7], (D, SHARED_FF), D ** -0.5, 0.125, ((1, 4),))
    shared_up = bell_draw(keys[8], (D, SHARED_FF), D ** -0.5, 0.125, ((1, 4),))
    shared_down = bell_draw(keys[9], (SHARED_FF, D), SHARED_FF ** -0.5, 0.25, ((1, 4),))
    return {"tokens": tokens, "norm_gain": norm_gain, "expert_ids": expert_ids, "route_weights": route_weights, "expert_gate": expert_gate, "expert_up": expert_up, "expert_down": expert_down, "shared_gate": shared_gate, "shared_up": shared_up, "shared_down": shared_down}


NORM_EPSILON = 1e-06

def rms_normed(tokens, norm_gain):
    as_float = tokens.astype(jnp.float32)
    inverse_rms = lax.rsqrt(lax.optimization_barrier(jnp.mean(as_float * as_float, axis=-1, keepdims=True)) + NORM_EPSILON)
    return (as_float * inverse_rms * norm_gain).astype(jnp.bfloat16)

def slot_numbers(expert_ids, block_rows, expert_count):
    expert_iota = jnp.arange(expert_count, dtype=jnp.int32)
    counts = lax.optimization_barrier(jnp.sum((expert_ids[:, :, None] == expert_iota[None, None, :]).astype(jnp.int32), axis=1))
    blocked = counts.reshape(-1, block_rows, expert_count)
    prefix = (jnp.cumsum(blocked, axis=1) - blocked).reshape(counts.shape)
    return jnp.take_along_axis(prefix, expert_ids, axis=1).astype(jnp.int32)

def half_output(gathered, gate_half, up_half, down_half):
    hidden = (jax.nn.silu(jnp.dot(gathered, gate_half, preferred_element_type=jnp.float32)) * jnp.dot(gathered, up_half, preferred_element_type=jnp.float32)).astype(jnp.bfloat16)
    rounded = jnp.dot(hidden, down_half, preferred_element_type=jnp.float32).astype(jnp.bfloat16)
    return lax.optimization_barrier(rounded).astype(jnp.float32)

def reference(tokens, norm_gain, expert_ids, route_weights, expert_gate, expert_up, expert_down, shared_gate, shared_up, shared_down):
    normed = rms_normed(tokens, norm_gain)
    token_count, model_width = tokens.shape
    block_rows = token_count // N_EP
    slot_index = slot_numbers(expert_ids, block_rows, EXPERTS)
    token_iota = jnp.arange(token_count, dtype=jnp.int32)
    source_block = jnp.broadcast_to((token_iota // block_rows)[:, None], expert_ids.shape).astype(jnp.int32)
    token_rows = jnp.broadcast_to(token_iota[:, None], expert_ids.shape).astype(jnp.int32)
    token_table = jnp.full((EXPERTS, N_EP, CAP), token_count, jnp.int32)
    token_table = token_table.at[expert_ids, source_block, slot_index].set(token_rows)
    weight_table = jnp.zeros((EXPERTS, N_EP, CAP), jnp.float32)
    weight_table = weight_table.at[expert_ids, source_block, slot_index].set(route_weights)
    padded = jnp.concatenate([normed, jnp.zeros((1, model_width), jnp.bfloat16)], axis=0)
    gate_pairs = expert_gate.reshape(EXPERTS, 2, model_width, EXP_HALF)
    up_pairs = expert_up.reshape(EXPERTS, 2, model_width, EXP_HALF)
    down_pairs = expert_down.reshape(EXPERTS, 2, EXP_HALF, model_width)

    def expert_step(running, inputs):
        gate_two, up_two, down_two, table_rows, table_weights = inputs
        flat_tokens = table_rows.reshape(-1)
        gathered = padded[flat_tokens]
        first = half_output(gathered, gate_two[0], up_two[0], down_two[0])
        second = half_output(gathered, gate_two[1], up_two[1], down_two[1])
        output = (first + second).astype(jnp.bfloat16)
        running = running.at[flat_tokens].add(output.astype(jnp.float32) * table_weights.reshape(-1)[:, None])
        return (running, None)
    start = jnp.zeros((token_count + 1, model_width), jnp.float32)
    routed, _ = lax.scan(expert_step, start, (gate_pairs, up_pairs, down_pairs, token_table, weight_table))
    shared_act = (jax.nn.silu(jnp.dot(normed, shared_gate, preferred_element_type=jnp.float32)) * jnp.dot(normed, shared_up, preferred_element_type=jnp.float32)).astype(jnp.bfloat16)
    shared_out = jnp.dot(shared_act, shared_down, preferred_element_type=jnp.float32)
    return (routed[:token_count] + shared_out).astype(jnp.bfloat16)
```

```python
import functools

import jax
import jax.numpy as jnp
from jax import lax
from jax.experimental import pallas as pl
from jax.experimental.pallas import tpu as pltpu
from jax.sharding import PartitionSpec as P

NORM_EPSILON = 1e-06


def swapped(block, axis, distance):
    count = lax.axis_size(axis)
    route = []
    for low in range(count):
        high = low | 1 << distance
        if high != low and high < count:
            route += [(low, high), (high, low)]
    return lax.ppermute(block, axis, route)


def routed_exchange(
    tokens,
    norm_gain,
    expert_ids,
    route_weights,
    expert_gate,
    expert_up,
    expert_down,
    shared_gate,
    shared_up,
    shared_down,
):
    ep_count = lax.axis_size("ep")
    tp_count = lax.axis_size("tp")
    pair_count = tp_count // 2
    tp_index = lax.axis_index("tp")
    column = tp_index // 2
    half_index = tp_index % 2
    token_count, model_width = tokens.shape
    top_count = expert_ids.shape[1]
    expert_count = ep_count * pair_count
    capacity = 2 * max(1, token_count * top_count // expert_count)
    half_cap = capacity // 2
    as_float = tokens.astype(jnp.float32)
    inverse_rms = lax.rsqrt(jnp.mean(as_float * as_float, axis=-1, keepdims=True) + NORM_EPSILON)
    normed = (as_float * inverse_rms * norm_gain).astype(jnp.bfloat16)
    expert_iota = jnp.arange(expert_count, dtype=jnp.int32)
    token_iota = jnp.arange(token_count, dtype=jnp.int32)
    counts = jnp.sum(
        (expert_ids[:, :, None] == expert_iota[None, None, :]).astype(jnp.bfloat16), axis=1
    )
    strict_lower = (token_iota[:, None] > token_iota[None, :]).astype(jnp.bfloat16)
    prefix = jnp.dot(strict_lower, counts, preferred_element_type=jnp.float32)
    slot_index = jnp.take_along_axis(prefix, expert_ids, axis=1).astype(jnp.int32)
    target = expert_ids // pair_count
    owner_column = expert_ids % pair_count
    is_mine = owner_column == column
    position = target * capacity + slot_index
    slot_iota = jnp.arange(ep_count * capacity, dtype=jnp.int32)
    matches = is_mine[None, :, :] & (position[None, :, :] == slot_iota[:, None, None])
    slot_taken = jnp.any(matches, axis=2)
    token_of_slot = jnp.sum(jnp.where(slot_taken, token_iota[None, :], 0), axis=1)
    filled = jnp.any(slot_taken, axis=1)
    buffer = jnp.where(
        filled[:, None], jnp.take(normed, token_of_slot, axis=0), jnp.zeros((), jnp.bfloat16)
    )
    buffer = buffer.reshape(ep_count, capacity, model_width)
    gate_local = expert_gate[0]
    up_local = expert_up[0]
    down_local = expert_down[0]
    received = lax.all_to_all(buffer, "ep", split_axis=0, concat_axis=0, tiled=True)
    flat_rows = received.reshape(-1, model_width)
    hidden = (
        jax.nn.silu(jnp.dot(flat_rows, gate_local, preferred_element_type=jnp.float32))
        * jnp.dot(flat_rows, up_local, preferred_element_type=jnp.float32)
    ).astype(jnp.bfloat16)
    partial_out = jnp.dot(hidden, down_local, preferred_element_type=jnp.float32).astype(
        jnp.bfloat16
    )
    partial_out = partial_out.reshape(received.shape[0], received.shape[1], model_width)
    kept_part = lax.dynamic_slice_in_dim(partial_out, half_index * half_cap, half_cap, 1)
    other_part = lax.dynamic_slice_in_dim(partial_out, (1 - half_index) * half_cap, half_cap, 1)
    partner_part = swapped(other_part, "tp", 0)
    expert_out = (kept_part.astype(jnp.float32) + partner_part.astype(jnp.float32)).astype(
        jnp.bfloat16
    )
    returned = lax.all_to_all(expert_out, "ep", split_axis=0, concat_axis=0, tiled=True)
    row_total = ep_count * half_cap
    flat_rows = returned.reshape(row_total, model_width).astype(jnp.float32)
    is_valid = is_mine & (slot_index // half_cap == half_index)
    row_index = jnp.where(is_valid, target * half_cap + slot_index % half_cap, -1)
    row_iota = jnp.arange(row_total, dtype=jnp.int32)
    hits = row_index[:, :, None] == row_iota[None, None, :]
    combine_table = jnp.sum(jnp.where(hits, route_weights[:, :, None], 0.0), axis=1)
    partial_routed = jnp.dot(
        combine_table,
        flat_rows,
        precision=lax.Precision.HIGHEST,
        preferred_element_type=jnp.float32,
    )
    routed = lax.psum_scatter(partial_routed, "tp", scatter_dimension=1, tiled=True)
    shared_act = (
        jax.nn.silu(jnp.dot(normed, shared_gate, preferred_element_type=jnp.float32))
        * jnp.dot(normed, shared_up, preferred_element_type=jnp.float32)
    ).astype(jnp.bfloat16)
    shared_out = jnp.dot(
        lax.all_gather(shared_act, "tp", axis=1, tiled=True),
        shared_down,
        preferred_element_type=jnp.float32,
    )
    return (routed + shared_out).astype(jnp.bfloat16)


MESH = pl.DeviceIdType.MESH
LANES = 128


def silu(v):
    return v / (1.0 + jnp.exp(-v))


def dense_kernel(
    ep_count, tp_count, minor, split,
    tok_ref, gain_ref, wt_ref, gate_hbm, up_hbm, down_hbm, sg_hbm, su_hbm, sd_hbm,
    out_ref,
    x_buf, y_buf, c_buf, xs_buf, xr_buf, zs_buf, zr_buf, ys_buf, yr_buf, fs_buf, fr_buf,
    acc, wt_all, sh_all, sh_out, gate, up, down, sg, su, sd,
    load_sem, wt_s, wt_r, sh_s, sh_r, y_s, u_s, d_s, z_r, x_s, x_r, c_s, c_r,
    yc_s, yc_r, rx_s, rx_r, rz_s, rz_r, ry_s, ry_r, f_s, f_r,
):
    major = ep_count // minor
    rows = tok_ref.shape[0]
    quarter = x_buf.shape[3]
    e = lax.axis_index("ep")
    t = lax.axis_index("tp")
    z = e // minor
    y = e % minor
    xi = t // 2
    c = t % 2
    t2 = 2 * (1 - xi) + c
    mate_x = {"tp": t2}
    mate_c = {"tp": 2 * xi + 1 - c}
    mate_y = {"ep": z * minor + 1 - y}
    z_up = {"ep": lax.rem(e + minor, ep_count)}
    z_down = {"ep": lax.rem(e + ep_count - minor, ep_count)}
    head_cols = pl.ds(0, split)
    rest_cols = pl.ds(split, quarter - split)

    def remote(src, dst, s, r, who):
        return pltpu.make_async_remote_copy(
            src_ref=src, dst_ref=dst, send_sem=s, recv_sem=r, device_id=who, device_id_type=MESH
        )

    loads = [
        pltpu.make_async_copy(a, b, load_sem.at[i])
        for i, (a, b) in enumerate(
            ((sg_hbm, sg), (su_hbm, su), (gate_hbm, gate), (up_hbm, up), (down_hbm, down), (sd_hbm, sd))
        )
    ]
    for load in loads:
        load.start()

    barrier = pltpu.get_barrier_semaphore()
    for k in range(1, ep_count):
        pl.semaphore_signal(barrier, inc=1, device_id={"ep": lax.rem(e + k, ep_count)}, device_id_type=MESH)
    for k in range(1, tp_count):
        pl.semaphore_signal(barrier, inc=1, device_id={"tp": lax.rem(t + k, tp_count)}, device_id_type=MESH)

    step = 16

    def norm_rows(i, carry):
        part = pl.ds(pl.multiple_of(i * step, step), step)
        v = tok_ref[part, :].astype(jnp.float32)
        r = lax.rsqrt(jnp.mean(v * v, axis=-1, keepdims=True) + NORM_EPSILON)
        n = (v * r * gain_ref[...]).astype(jnp.bfloat16)
        for q in range(tp_count):
            x_buf[e, q, part, :] = n[:, q * quarter : (q + 1) * quarter]
        return carry

    lax.fori_loop(0, rows // step, norm_rows, 0)
    pl.semaphore_wait(barrier, ep_count + tp_count - 2)

    def wt_copy(k, slot, who):
        src = wt_ref if slot is None else wt_all.at[slot]
        dst = wt_all.at[e if slot is None else slot]
        return remote(src, dst, wt_s.at[k], wt_r.at[k], {"ep": who})

    def main_of(g):
        return x_buf.at[g, t]

    def rest_of(g):
        return x_buf.at[g, t2, :, rest_cols]

    def line(g, s, who):
        return (
            remote(main_of(g), main_of(g), s.at[g, 0], z_r.at[g, 0], who),
            remote(rest_of(g), rest_of(g), s.at[g, 1], z_r.at[g, 1], who),
        )

    def x_copy(g):
        ref = x_buf.at[g, t, :, head_cols]
        return remote(ref, ref, x_s.at[g], x_r.at[g], mate_x)

    def x_arrival(g):
        ref = x_buf.at[g, t2, :, head_cols]
        return remote(ref, ref, x_s.at[g], x_r.at[g], mate_x)

    def c_copies(g, lane):
        main, other = 2 * xi + lane, 2 * (1 - xi) + lane
        refs = (x_buf.at[g, main], x_buf.at[g, other, :, rest_cols], x_buf.at[g, other, :, head_cols])
        return [remote(r, r, c_s.at[g, i], c_r.at[g, i], mate_c) for i, r in enumerate(refs)]

    def order(j):
        k = jnp.minimum(z, major - 1 - z)
        d = (j + 1) // 2
        near = jnp.where(j % 2 == 1, z - d, z + d)
        far = jnp.where(z <= major - 1 - z, j, major - 1 - j)
        return jnp.where(j <= 2 * k, near, far)

    def slot_group(i):
        p = order(i // 2)
        yy = jnp.where(i % 2 == 0, y, 1 - y)
        return p, p * minor + yy

    def forward(p, g):
        @pl.when((p <= z) & (z < major - 1))
        def _():
            for copy in line(g, u_s, z_up):
                copy.start()

        @pl.when((p >= z) & (z > 0))
        def _():
            for copy in line(g, d_s, z_down):
                copy.start()

    for copy in line(e, y_s, mate_y):
        copy.start()
    for k in range(1, ep_count):
        wt_copy(k, None, lax.rem(e + k, ep_count)).start()
    wt_all[e] = wt_ref[...]
    forward(z, e)

    loads[0].wait()
    loads[1].wait()
    sg_sum = jnp.zeros((rows, sg.shape[1]), jnp.float32)
    su_sum = jnp.zeros((rows, sg.shape[1]), jnp.float32)
    for q in range(tp_count):
        band = pl.ds(q * quarter, quarter)
        sg_sum += jnp.dot(x_buf[e, q], sg[band, :], preferred_element_type=jnp.float32)
        su_sum += jnp.dot(x_buf[e, q], su[band, :], preferred_element_type=jnp.float32)
    sh_all[t] = (silu(sg_sum) * su_sum).astype(jnp.bfloat16)

    def sh_copy(k, slot, who):
        return remote(sh_all.at[slot], sh_all.at[slot], sh_s.at[k], sh_r.at[k], {"tp": who})

    for k in range(1, tp_count):
        sh_copy(k, t, lax.rem(t + k, tp_count)).start()
    for load in loads[2:5]:
        load.wait()
    for k in range(1, ep_count):
        wt_copy(k, lax.rem(e + ep_count - k, ep_count), e).wait_recv()

    expert = e * (tp_count // 2) + xi
    expert_mask = lax.broadcasted_iota(jnp.int32, wt_ref.shape, 0) == expert
    eye = lax.broadcasted_iota(jnp.int32, (rows, rows), 0) == lax.broadcasted_iota(
        jnp.int32, (rows, rows), 1
    )

    def compute(g):
        row = jnp.sum(jnp.where(expert_mask, wt_all[g], 0.0), axis=0, keepdims=True)
        weight = jnp.sum(jnp.where(eye, row, 0.0), axis=1, keepdims=True)
        ff = gate.shape[1]
        g_sum = jnp.zeros((rows, ff), jnp.float32)
        u_sum = jnp.zeros((rows, ff), jnp.float32)
        for q in range(tp_count):
            band = pl.ds(q * quarter, quarter)
            g_sum += jnp.dot(x_buf[g, q], gate[band, :], preferred_element_type=jnp.float32)
            u_sum += jnp.dot(x_buf[g, q], up[band, :], preferred_element_type=jnp.float32)
        act = (silu(g_sum) * u_sum).astype(jnp.bfloat16)
        for q in range(tp_count):
            part = jnp.dot(
                act, down[:, q * quarter : (q + 1) * quarter], preferred_element_type=jnp.float32
            )
            y_buf[g, q] = (part * weight).astype(jnp.bfloat16)

    def yc_copy(g, k):
        return remote(
            y_buf.at[g, 2 * k + 1 - c], c_buf.at[g, k], yc_s.at[g, k], yc_r.at[g, k], mate_c
        )

    def rx_copy(g):
        return remote(xs_buf.at[g], xr_buf.at[g], rx_s.at[g], rx_r.at[g], mate_x)

    total = ep_count

    def main_step(i, carry):
        @pl.when((i >= 1) & (i < total))
        def _():
            p, g = slot_group(i)
            for copy in line(g, u_s, z_up):
                copy.wait_recv()
            forward(p, g)
            x_copy(g).start()
            ours = c_copies(g, c)
            ours[0].start()
            ours[1].start()

        @pl.when((i >= 1) & (i <= total))
        def _():
            _, g = slot_group(i - 1)

            @pl.when(i >= 2)
            def _():
                x_arrival(g).wait_recv()
                c_copies(g, c)[2].start()
                for copy in c_copies(g, 1 - c):
                    copy.wait_recv()

            compute(g)
            for k in range(2):
                yc_copy(g, k).start()

        @pl.when(i >= 2)
        def _():
            _, g = slot_group(i - 2)
            for k in range(2):
                yc_copy(g, k).wait_recv()
            xs_buf[g] = (
                y_buf[g, t2, :, head_cols].astype(jnp.float32)
                + c_buf[g, 1 - xi, :, head_cols].astype(jnp.float32)
            ).astype(jnp.bfloat16)
            rx_copy(g).start()

        return carry

    lax.fori_loop(0, total + 2, main_step, 0)

    loads[5].wait()
    for k in range(1, tp_count):
        sh_copy(k, lax.rem(t + tp_count - k, tp_count), t).wait_recv()
    shared = jnp.zeros((rows, quarter), jnp.float32)
    width = sg.shape[1]
    for q in range(tp_count):
        shared += jnp.dot(
            sh_all[q], sd[q * width : (q + 1) * width, :], preferred_element_type=jnp.float32
        )
    sh_out[...] = shared

    def rz_copy(g, lane, who):
        return remote(zs_buf.at[g], zr_buf.at[lane, g], rz_s.at[g], rz_r.at[lane, g], who)

    def gather_sum(p, g):
        rx_copy(g).wait_recv()
        mine = y_buf[g, t].astype(jnp.float32) + c_buf[g, xi].astype(jnp.float32)
        acc[:, :split] = mine[:, :split] + xr_buf[g].astype(jnp.float32)
        acc[:, split:quarter] = mine[:, split:]
        acc[:, quarter:] = y_buf[g, t2, :, rest_cols].astype(jnp.float32) + c_buf[
            g, 1 - xi, :, rest_cols
        ].astype(jnp.float32)

        @pl.when((p >= z) & (z > 0))
        def _():
            rz_copy(g, 0, z_up).wait_recv()
            acc[...] += zr_buf[0, g].astype(jnp.float32)

        @pl.when((p <= z) & (z < major - 1))
        def _():
            rz_copy(g, 1, z_up).wait_recv()
            acc[...] += zr_buf[1, g].astype(jnp.float32)

    def sum_step(i, carry):
        q = i // 2
        ups = major - 1 - z
        low = jnp.where(q < ups, z + 1 + q, z - 1 - (q - ups))
        high = jnp.where(q < z, z - 1 - q, z + 1 + (q - z))
        p = jnp.where(2 * z < major, low, high)
        g = p * minor + jnp.where(i % 2 == 0, y, 1 - y)
        gather_sum(p, g)
        zs_buf[g] = acc[...].astype(jnp.bfloat16)

        @pl.when(p > z)
        def _():
            rz_copy(g, 0, z_up).start()

        @pl.when(p < z)
        def _():
            rz_copy(g, 1, z_down).start()

        return carry

    lax.fori_loop(0, ep_count - minor, sum_step, 0)

    y_copy = remote(ys_buf, yr_buf, ry_s, ry_r, mate_y)
    gather_sum(z, z * minor + 1 - y)
    ys_buf[...] = acc[...].astype(jnp.bfloat16)
    y_copy.start()
    gather_sum(z, e)
    y_copy.wait_recv()
    final = acc[...] + yr_buf[...].astype(jnp.float32)
    f_copy = remote(fs_buf, fr_buf, f_s, f_r, mate_x)
    fs_buf[...] = final[:, quarter:].astype(jnp.bfloat16)
    f_copy.start()
    out_ref[:, :split] = (final[:, :split] + sh_out[:, :split]).astype(jnp.bfloat16)
    f_copy.wait_recv()
    out_ref[:, split:] = (
        final[:, split:quarter] + fr_buf[...].astype(jnp.float32) + sh_out[:, split:]
    ).astype(jnp.bfloat16)

    f_copy.wait_send()
    y_copy.wait_send()
    for copy in line(e, y_s, mate_y):
        copy.wait_send()
    for k in range(1, ep_count):
        wt_copy(k, None, lax.rem(e + k, ep_count)).wait_send()
    for k in range(1, tp_count):
        sh_copy(k, t, lax.rem(t + k, tp_count)).wait_send()

    def drain(i, carry):
        p, g = slot_group(i)

        @pl.when((p <= z) & (z < major - 1))
        def _():
            for copy in line(g, u_s, z_up):
                copy.wait_send()

        @pl.when((p >= z) & (z > 0))
        def _():
            for copy in line(g, d_s, z_down):
                copy.wait_send()

        @pl.when(i > 0)
        def _():
            x_copy(g).wait_send()
            for copy in c_copies(g, c):
                copy.wait_send()

        for k in range(2):
            yc_copy(g, k).wait_send()
        rx_copy(g).wait_send()

        @pl.when(p != z)
        def _():
            rz_copy(g, 0, z_up).wait_send()

        return carry

    lax.fori_loop(0, total, drain, 0)


def dense_exchange(
    tokens, norm_gain, expert_ids, route_weights, expert_gate, expert_up, expert_down,
    shared_gate, shared_up, shared_down,
):
    ep_count = lax.axis_size("ep")
    tp_count = lax.axis_size("tp")
    minor = 1 << (ep_count.bit_length() - 1) // 2
    rows, width = tokens.shape
    quarter = width // tp_count
    split = quarter * 3 // 4 // LANES * LANES
    expert_count = ep_count * tp_count // 2
    wide = quarter + quarter - split
    expert_iota = jnp.arange(expert_count, dtype=jnp.int32)
    table = jnp.sum(
        jnp.where(
            expert_ids[None, :, :] == expert_iota[:, None, None], route_weights[None, :, :], 0.0
        ),
        axis=2,
    )
    ff = expert_gate.shape[2]
    share = shared_gate.shape[1]
    bf16, f32 = jnp.bfloat16, jnp.float32
    dma = pltpu.SemaphoreType.DMA
    vmem = pl.BlockSpec(memory_space=pltpu.VMEM)
    anywhere = pl.BlockSpec(memory_space=pl.ANY)
    n = ep_count
    return pl.pallas_call(
        functools.partial(dense_kernel, ep_count, tp_count, minor, split),
        out_shape=jax.ShapeDtypeStruct((rows, quarter), bf16),
        in_specs=[vmem] * 3 + [anywhere] * 6,
        out_specs=vmem,
        scratch_shapes=[
            pltpu.VMEM((n, tp_count, rows, quarter), bf16),
            pltpu.VMEM((n, tp_count, rows, quarter), bf16),
            pltpu.VMEM((n, 2, rows, quarter), bf16),
            pltpu.VMEM((n, rows, split), bf16),
            pltpu.VMEM((n, rows, split), bf16),
            pltpu.VMEM((n, rows, wide), bf16),
            pltpu.VMEM((2, n, rows, wide), bf16),
            pltpu.VMEM((rows, wide), bf16),
            pltpu.VMEM((rows, wide), bf16),
            pltpu.VMEM((rows, quarter - split), bf16),
            pltpu.VMEM((rows, quarter - split), bf16),
            pltpu.VMEM((rows, wide), f32),
            pltpu.VMEM((n, expert_count, rows), f32),
            pltpu.VMEM((tp_count, rows, share), bf16),
            pltpu.VMEM((rows, quarter), f32),
            pltpu.VMEM((width, ff), bf16),
            pltpu.VMEM((width, ff), bf16),
            pltpu.VMEM((ff, width), bf16),
            pltpu.VMEM((width, share), bf16),
            pltpu.VMEM((width, share), bf16),
            pltpu.VMEM((share * tp_count, quarter), bf16),
            dma((6,)), dma((n,)), dma((n,)), dma((tp_count,)), dma((tp_count,)),
            dma((n, 2)), dma((n, 2)), dma((n, 2)), dma((n, 2)),
            dma((n,)), dma((n,)), dma((n, 3)), dma((n, 3)),
            dma((n, 2)), dma((n, 2)), dma((n,)), dma((n,)),
            dma((n,)), dma((2, n)), dma, dma, dma, dma,
        ],
        compiler_params=pltpu.CompilerParams(
            collective_id=0, has_side_effects=True, vmem_limit_bytes=60 << 20
        ),
        name="dense_moe",
    )(
        tokens, norm_gain.reshape(1, width), table, expert_gate[0], expert_up[0], expert_down[0],
        shared_gate, shared_up, shared_down,
    )


def local(tokens, *rest):
    ep_count = lax.axis_size("ep")
    pair_count = lax.axis_size("tp") // 2
    dense_bytes = 4 * ep_count * tokens.size * tokens.dtype.itemsize
    minor = 1 << (ep_count.bit_length() - 1) // 2
    if pair_count == 2 and minor == 2 and dense_bytes <= 24 << 20:
        return dense_exchange(tokens, *rest)
    return routed_exchange(tokens, *rest)


def solution(mesh):
    return jax.shard_map(
        local,
        mesh=mesh,
        in_specs=(
            P("ep", None),
            P(),
            P("ep", None),
            P("ep", None),
            P(("ep", "tp"), None, None),
            P(("ep", "tp"), None, None),
            P(("ep", "tp"), None, None),
            P(None, "tp"),
            P(None, "tp"),
            P(None, "tp"),
        ),
        out_specs=P("ep", "tp"),
        check_vma=False,
    )
```

```python
import functools

import jax
import jax.numpy as jnp
from jax import lax
from jax.experimental import pallas as pl
from jax.experimental.pallas import tpu as pltpu
from jax.sharding import PartitionSpec as P

NORM_EPSILON = 1e-06


def swapped(block, axis, distance):
    count = lax.axis_size(axis)
    route = []
    for low in range(count):
        high = low | 1 << distance
        if high != low and high < count:
            route += [(low, high), (high, low)]
    return lax.ppermute(block, axis, route)


def routed_exchange(
    tokens,
    norm_gain,
    expert_ids,
    route_weights,
    expert_gate,
    expert_up,
    expert_down,
    shared_gate,
    shared_up,
    shared_down,
):
    ep_count = lax.axis_size("ep")
    tp_count = lax.axis_size("tp")
    pair_count = tp_count // 2
    tp_index = lax.axis_index("tp")
    column = tp_index // 2
    half_index = tp_index % 2
    token_count, model_width = tokens.shape
    top_count = expert_ids.shape[1]
    expert_count = ep_count * pair_count
    capacity = 2 * max(1, token_count * top_count // expert_count)
    half_cap = capacity // 2
    as_float = tokens.astype(jnp.float32)
    inverse_rms = lax.rsqrt(jnp.mean(as_float * as_float, axis=-1, keepdims=True) + NORM_EPSILON)
    normed = (as_float * inverse_rms * norm_gain).astype(jnp.bfloat16)
    expert_iota = jnp.arange(expert_count, dtype=jnp.int32)
    token_iota = jnp.arange(token_count, dtype=jnp.int32)
    counts = jnp.sum(
        (expert_ids[:, :, None] == expert_iota[None, None, :]).astype(jnp.bfloat16), axis=1
    )
    strict_lower = (token_iota[:, None] > token_iota[None, :]).astype(jnp.bfloat16)
    prefix = jnp.dot(strict_lower, counts, preferred_element_type=jnp.float32)
    slot_index = jnp.take_along_axis(prefix, expert_ids, axis=1).astype(jnp.int32)
    target = expert_ids // pair_count
    owner_column = expert_ids % pair_count
    is_mine = owner_column == column
    position = target * capacity + slot_index
    slot_iota = jnp.arange(ep_count * capacity, dtype=jnp.int32)
    matches = is_mine[None, :, :] & (position[None, :, :] == slot_iota[:, None, None])
    slot_taken = jnp.any(matches, axis=2)
    token_of_slot = jnp.sum(jnp.where(slot_taken, token_iota[None, :], 0), axis=1)
    filled = jnp.any(slot_taken, axis=1)
    buffer = jnp.where(
        filled[:, None], jnp.take(normed, token_of_slot, axis=0), jnp.zeros((), jnp.bfloat16)
    )
    buffer = buffer.reshape(ep_count, capacity, model_width)
    gate_local = expert_gate[0]
    up_local = expert_up[0]
    down_local = expert_down[0]
    received = lax.all_to_all(buffer, "ep", split_axis=0, concat_axis=0, tiled=True)
    flat_rows = received.reshape(-1, model_width)
    hidden = (
        jax.nn.silu(jnp.dot(flat_rows, gate_local, preferred_element_type=jnp.float32))
        * jnp.dot(flat_rows, up_local, preferred_element_type=jnp.float32)
    ).astype(jnp.bfloat16)
    partial_out = jnp.dot(hidden, down_local, preferred_element_type=jnp.float32).astype(
        jnp.bfloat16
    )
    partial_out = partial_out.reshape(received.shape[0], received.shape[1], model_width)
    kept_part = lax.dynamic_slice_in_dim(partial_out, half_index * half_cap, half_cap, 1)
    other_part = lax.dynamic_slice_in_dim(partial_out, (1 - half_index) * half_cap, half_cap, 1)
    partner_part = swapped(other_part, "tp", 0)
    expert_out = (kept_part.astype(jnp.float32) + partner_part.astype(jnp.float32)).astype(
        jnp.bfloat16
    )
    returned = lax.all_to_all(expert_out, "ep", split_axis=0, concat_axis=0, tiled=True)
    row_total = ep_count * half_cap
    flat_rows = returned.reshape(row_total, model_width).astype(jnp.float32)
    is_valid = is_mine & (slot_index // half_cap == half_index)
    row_index = jnp.where(is_valid, target * half_cap + slot_index % half_cap, -1)
    row_iota = jnp.arange(row_total, dtype=jnp.int32)
    hits = row_index[:, :, None] == row_iota[None, None, :]
    combine_table = jnp.sum(jnp.where(hits, route_weights[:, :, None], 0.0), axis=1)
    partial_routed = jnp.dot(
        combine_table,
        flat_rows,
        precision=lax.Precision.HIGHEST,
        preferred_element_type=jnp.float32,
    )
    routed = lax.psum_scatter(partial_routed, "tp", scatter_dimension=1, tiled=True)
    shared_act = (
        jax.nn.silu(jnp.dot(normed, shared_gate, preferred_element_type=jnp.float32))
        * jnp.dot(normed, shared_up, preferred_element_type=jnp.float32)
    ).astype(jnp.bfloat16)
    shared_out = jnp.dot(
        lax.all_gather(shared_act, "tp", axis=1, tiled=True),
        shared_down,
        preferred_element_type=jnp.float32,
    )
    return (routed + shared_out).astype(jnp.bfloat16)


MESH = pl.DeviceIdType.MESH
LANES = 128


def silu(v):
    return v / (1.0 + jnp.exp(-v))


def dense_kernel(
    ep_count, tp_count, minor, split,
    tok_ref, gain_ref, wt_ref, gate_hbm, up_hbm, down_hbm, sg_hbm, su_hbm, sd_hbm,
    out_ref,
    x_buf, y_buf, c_buf, xs_buf, xr_buf, ysa_buf, yra_buf, zsa_buf, zra_buf, zs_buf, zr_buf,
    ys_buf, yr_buf, fs_buf, fr_buf,
    acc, wt_all, sh_all, sh_out, gate, up, down, sg, su, sd,
    load_sem, wt_s, wt_r, sh_s, sh_r, y_s, u_s, d_s, z_r, x_s, x_r, c_s, c_r,
    ya_s, ya_r, yc_s, yc_r, rx_s, rx_r, rya_s, rya_r, rza_s, rza_r, rz_s, rz_r, ry_s, ry_r,
    f_s, f_r,
):
    major = ep_count // minor
    rows = tok_ref.shape[0]
    quarter = x_buf.shape[3]
    e = lax.axis_index("ep")
    t = lax.axis_index("tp")
    z = e // minor
    y = e % minor
    xi = t // 2
    c = t % 2
    t2 = 2 * (1 - xi) + c
    mate_x = {"tp": t2}
    mate_c = {"tp": 2 * xi + 1 - c}
    mate_y = {"ep": z * minor + 1 - y}
    z_up = {"ep": lax.rem(e + minor, ep_count)}
    z_down = {"ep": lax.rem(e + ep_count - minor, ep_count)}
    head_cols = pl.ds(0, split)
    rest_cols = pl.ds(split, quarter - split)

    def remote(src, dst, s, r, who):
        return pltpu.make_async_remote_copy(
            src_ref=src, dst_ref=dst, send_sem=s, recv_sem=r, device_id=who, device_id_type=MESH
        )

    loads = [
        pltpu.make_async_copy(a, b, load_sem.at[i])
        for i, (a, b) in enumerate(
            ((sg_hbm, sg), (su_hbm, su), (gate_hbm, gate), (up_hbm, up), (down_hbm, down), (sd_hbm, sd))
        )
    ]
    for load in loads:
        load.start()

    barrier = pltpu.get_barrier_semaphore()
    for k in range(1, ep_count):
        pl.semaphore_signal(barrier, inc=1, device_id={"ep": lax.rem(e + k, ep_count)}, device_id_type=MESH)
    for k in range(1, tp_count):
        pl.semaphore_signal(barrier, inc=1, device_id={"tp": lax.rem(t + k, tp_count)}, device_id_type=MESH)

    step = 16

    def norm_rows(i, carry):
        part = pl.ds(pl.multiple_of(i * step, step), step)
        v = tok_ref[part, :].astype(jnp.float32)
        r = lax.rsqrt(jnp.mean(v * v, axis=-1, keepdims=True) + NORM_EPSILON)
        n = (v * r * gain_ref[...]).astype(jnp.bfloat16)
        for q in range(tp_count):
            x_buf[e, q, part, :] = n[:, q * quarter : (q + 1) * quarter]
        return carry

    lax.fori_loop(0, rows // step, norm_rows, 0)
    pl.semaphore_wait(barrier, ep_count + tp_count - 2)

    def wt_copy(k, slot, who):
        src = wt_ref if slot is None else wt_all.at[slot]
        dst = wt_all.at[e if slot is None else slot]
        return remote(src, dst, wt_s.at[k], wt_r.at[k], {"ep": who})

    def head_of(g, q):
        return x_buf.at[g, q, :, head_cols]

    def rest_of(g, q):
        return x_buf.at[g, q, :, rest_cols]

    def line_head(g, s, who):
        return (remote(head_of(g, t), head_of(g, t), s.at[g, 0], z_r.at[g, 0], who),)

    def line_rest(g, s, who):
        return (
            remote(rest_of(g, t), rest_of(g, t), s.at[g, 1], z_r.at[g, 1], who),
            remote(rest_of(g, t2), rest_of(g, t2), s.at[g, 2], z_r.at[g, 2], who),
        )

    def y_copy_head(g):
        return remote(head_of(g, t), head_of(g, t), ya_s.at[g], ya_r.at[g], mate_y)

    def x_copy(g):
        ref = x_buf.at[g, t, :, head_cols]
        return remote(ref, ref, x_s.at[g], x_r.at[g], mate_x)

    def x_arrival(g):
        ref = x_buf.at[g, t2, :, head_cols]
        return remote(ref, ref, x_s.at[g], x_r.at[g], mate_x)

    def c_copies(g, lane):
        main, other = 2 * xi + lane, 2 * (1 - xi) + lane
        refs = (head_of(g, main), rest_of(g, main), rest_of(g, other), head_of(g, other))
        return [remote(r, r, c_s.at[g, i], c_r.at[g, i], mate_c) for i, r in enumerate(refs)]

    def order(j):
        k = jnp.minimum(z, major - 1 - z)
        d = (j + 1) // 2
        near = jnp.where(j % 2 == 1, z - d, z + d)
        far = jnp.where(z <= major - 1 - z, j, major - 1 - j)
        return jnp.where(j <= 2 * k, near, far)

    def slot_group(i):
        p = order(i // 2)
        yy = jnp.where(i % 2 == 0, y, 1 - y)
        return p, p * minor + yy

    def forward(p, g, pieces):
        @pl.when((p <= z) & (z < major - 1))
        def _():
            for copy in pieces(g, u_s, z_up):
                copy.start()

        @pl.when((p >= z) & (z > 0))
        def _():
            for copy in pieces(g, d_s, z_down):
                copy.start()

    for copy in line_rest(e, y_s, mate_y):
        copy.start()
    forward(z, e, line_head)
    y_copy_head(e).start()
    for k in range(1, ep_count):
        wt_copy(k, None, lax.rem(e + k, ep_count)).start()
    wt_all[e] = wt_ref[...]
    forward(z, e, line_rest)

    loads[0].wait()
    loads[1].wait()
    sg_sum = jnp.zeros((rows, sg.shape[1]), jnp.float32)
    su_sum = jnp.zeros((rows, sg.shape[1]), jnp.float32)
    for q in range(tp_count):
        band = pl.ds(q * quarter, quarter)
        sg_sum += jnp.dot(x_buf[e, q], sg[band, :], preferred_element_type=jnp.float32)
        su_sum += jnp.dot(x_buf[e, q], su[band, :], preferred_element_type=jnp.float32)
    sh_all[t] = (silu(sg_sum) * su_sum).astype(jnp.bfloat16)

    def sh_copy(k, slot, who):
        return remote(sh_all.at[slot], sh_all.at[slot], sh_s.at[k], sh_r.at[k], {"tp": who})

    for k in range(1, tp_count):
        sh_copy(k, t, lax.rem(t + k, tp_count)).start()
    for load in loads[2:5]:
        load.wait()
    for k in range(1, ep_count):
        wt_copy(k, lax.rem(e + ep_count - k, ep_count), e).wait_recv()

    expert = e * (tp_count // 2) + xi
    expert_mask = lax.broadcasted_iota(jnp.int32, wt_ref.shape, 0) == expert
    eye = lax.broadcasted_iota(jnp.int32, (rows, rows), 0) == lax.broadcasted_iota(
        jnp.int32, (rows, rows), 1
    )

    def compute(g):
        row = jnp.sum(jnp.where(expert_mask, wt_all[g], 0.0), axis=0, keepdims=True)
        weight = jnp.sum(jnp.where(eye, row, 0.0), axis=1, keepdims=True)
        ff = gate.shape[1]
        g_sum = jnp.zeros((rows, ff), jnp.float32)
        u_sum = jnp.zeros((rows, ff), jnp.float32)
        for q in range(tp_count):
            band = pl.ds(q * quarter, quarter)
            g_sum += jnp.dot(x_buf[g, q], gate[band, :], preferred_element_type=jnp.float32)
            u_sum += jnp.dot(x_buf[g, q], up[band, :], preferred_element_type=jnp.float32)
        act = (silu(g_sum) * u_sum).astype(jnp.bfloat16)
        for q in range(tp_count):
            part = jnp.dot(
                act, down[:, q * quarter : (q + 1) * quarter], preferred_element_type=jnp.float32
            )
            y_buf[g, q] = (part * weight).astype(jnp.bfloat16)

    def yc_copy(g, k):
        return remote(
            y_buf.at[g, 2 * k + 1 - c], c_buf.at[g, k], yc_s.at[g, k], yc_r.at[g, k], mate_c
        )

    def rx_copy(g):
        return remote(xs_buf.at[g], xr_buf.at[g], rx_s.at[g], rx_r.at[g], mate_x)

    def rya_copy(p):
        return remote(ysa_buf.at[p], yra_buf.at[p], rya_s.at[p], rya_r.at[p], mate_y)

    total = ep_count

    def head_sum(g):
        return (
            y_buf[g, t, :, head_cols].astype(jnp.float32)
            + c_buf[g, xi, :, head_cols].astype(jnp.float32)
            + xr_buf[g].astype(jnp.float32)
        )

    def main_step(i, carry):
        @pl.when((i >= 1) & (i < total))
        def _():
            p, g = slot_group(i)
            ours = c_copies(g, c)

            @pl.when(i % 2 == 0)
            def _():
                line_head(g, u_s, z_up)[0].wait_recv()
                forward(p, g, line_head)
                y_copy_head(g).start()
                x_copy(g).start()
                ours[0].start()

            for copy in line_rest(g, u_s, z_up):
                copy.wait_recv()
            forward(p, g, line_rest)
            ours[1].start()
            ours[2].start()

        @pl.when((i >= 2) & (i <= total) & (i % 2 == 0))
        def _():
            _, g = slot_group(i - 1)
            y_copy_head(g).wait_recv()
            x_copy(g).start()
            c_copies(g, c)[0].start()

        @pl.when((i >= 2) & (i <= total + 1))
        def _():
            _, g = slot_group(i - 2)

            @pl.when(i >= 3)
            def _():
                x_arrival(g).wait_recv()
                c_copies(g, c)[3].start()
                for copy in c_copies(g, 1 - c):
                    copy.wait_recv()

            compute(g)
            for k in range(2):
                yc_copy(g, k).start()

        @pl.when((i >= 3) & (i <= total + 2))
        def _():
            _, g = slot_group(i - 3)
            for k in range(2):
                yc_copy(g, k).wait_recv()
            xs_buf[g] = (
                y_buf[g, t2, :, head_cols].astype(jnp.float32)
                + c_buf[g, 1 - xi, :, head_cols].astype(jnp.float32)
            ).astype(jnp.bfloat16)
            rx_copy(g).start()

        @pl.when((i >= 5) & (i % 2 == 1))
        def _():
            p, g = slot_group(i - 4)
            rx_copy(g).wait_recv()
            ysa_buf[p] = head_sum(g).astype(jnp.bfloat16)
            rya_copy(p).start()

        return carry

    lax.fori_loop(0, total + 4, main_step, 0)

    loads[5].wait()
    for k in range(1, tp_count):
        sh_copy(k, lax.rem(t + tp_count - k, tp_count), t).wait_recv()
    shared = jnp.zeros((rows, quarter), jnp.float32)
    width = sg.shape[1]
    for q in range(tp_count):
        shared += jnp.dot(
            sh_all[q], sd[q * width : (q + 1) * width, :], preferred_element_type=jnp.float32
        )
    sh_out[...] = shared

    def rz_copy(g, lane, who):
        return remote(zs_buf.at[g], zr_buf.at[lane, g], rz_s.at[g], rz_r.at[lane, g], who)

    def rza_copy(p, lane, who):
        return remote(zsa_buf.at[p], zra_buf.at[lane, p], rza_s.at[p], rza_r.at[lane, p], who)

    def sum_rest(p, g):
        acc[:, split:quarter] = y_buf[g, t, :, rest_cols].astype(jnp.float32) + c_buf[
            g, xi, :, rest_cols
        ].astype(jnp.float32)
        acc[:, quarter:] = y_buf[g, t2, :, rest_cols].astype(jnp.float32) + c_buf[
            g, 1 - xi, :, rest_cols
        ].astype(jnp.float32)

        @pl.when((p >= z) & (z > 0))
        def _():
            rz_copy(g, 0, z_up).wait_recv()
            acc[:, split:] += zr_buf[0, g].astype(jnp.float32)

        @pl.when((p <= z) & (z < major - 1))
        def _():
            rz_copy(g, 1, z_up).wait_recv()
            acc[:, split:] += zr_buf[1, g].astype(jnp.float32)

    def sum_head(p, g):
        rx_copy(g).wait_recv()
        rya_copy(p).wait_recv()
        acc[:, :split] = head_sum(g) + yra_buf[p].astype(jnp.float32)

        @pl.when((p >= z) & (z > 0))
        def _():
            rza_copy(p, 0, z_up).wait_recv()
            acc[:, :split] += zra_buf[0, p].astype(jnp.float32)

        @pl.when((p <= z) & (z < major - 1))
        def _():
            rza_copy(p, 1, z_up).wait_recv()
            acc[:, :split] += zra_buf[1, p].astype(jnp.float32)

    def sum_step(q, carry):
        ups = major - 1 - z
        low = jnp.where(q < ups, z + 1 + q, z - 1 - (q - ups))
        high = jnp.where(q < z, z - 1 - q, z + 1 + (q - z))
        p = jnp.where(2 * z < major, low, high)

        def send(copy, key):
            @pl.when(p > z)
            def _():
                copy(key, 0, z_up).start()

            @pl.when(p < z)
            def _():
                copy(key, 1, z_down).start()

        for yy in (1 - y, y):
            g = p * minor + yy
            sum_rest(p, g)
            zs_buf[g] = acc[:, split:].astype(jnp.bfloat16)
            send(rz_copy, g)
        sum_head(p, p * minor + y)
        zsa_buf[p] = acc[:, :split].astype(jnp.bfloat16)
        send(rza_copy, p)
        return carry

    lax.fori_loop(0, major - 1, sum_step, 0)

    y_copy = remote(ys_buf, yr_buf, ry_s, ry_r, mate_y)
    sum_rest(z, z * minor + 1 - y)
    ys_buf[...] = acc[:, split:].astype(jnp.bfloat16)
    y_copy.start()
    sum_rest(z, e)
    sum_head(z, e)
    y_copy.wait_recv()
    acc[:, split:] += yr_buf[...].astype(jnp.float32)
    final = acc[...]
    f_copy = remote(fs_buf, fr_buf, f_s, f_r, mate_x)
    fs_buf[...] = final[:, quarter:].astype(jnp.bfloat16)
    f_copy.start()
    out_ref[:, :split] = (final[:, :split] + sh_out[:, :split]).astype(jnp.bfloat16)
    f_copy.wait_recv()
    out_ref[:, split:] = (
        final[:, split:quarter] + fr_buf[...].astype(jnp.float32) + sh_out[:, split:]
    ).astype(jnp.bfloat16)

    f_copy.wait_send()
    y_copy.wait_send()
    for copy in line_rest(e, y_s, mate_y):
        copy.wait_send()
    for k in range(1, ep_count):
        wt_copy(k, None, lax.rem(e + k, ep_count)).wait_send()
    for k in range(1, tp_count):
        sh_copy(k, t, lax.rem(t + k, tp_count)).wait_send()

    def drain(i, carry):
        p, g = slot_group(i)

        def sent(pieces):
            @pl.when((p <= z) & (z < major - 1))
            def _():
                for copy in pieces(g, u_s, z_up):
                    copy.wait_send()

            @pl.when((p >= z) & (z > 0))
            def _():
                for copy in pieces(g, d_s, z_down):
                    copy.wait_send()

        sent(line_rest)

        @pl.when(i % 2 == 0)
        def _():
            sent(line_head)
            y_copy_head(g).wait_send()

            @pl.when(p != z)
            def _():
                rza_copy(p, 0, z_up).wait_send()

        @pl.when(i % 2 == 1)
        def _():
            rya_copy(p).wait_send()

        @pl.when(i > 0)
        def _():
            x_copy(g).wait_send()
            for copy in c_copies(g, c):
                copy.wait_send()

        for k in range(2):
            yc_copy(g, k).wait_send()
        rx_copy(g).wait_send()

        @pl.when(p != z)
        def _():
            rz_copy(g, 0, z_up).wait_send()

        return carry

    lax.fori_loop(0, total, drain, 0)


def dense_exchange(
    tokens, norm_gain, expert_ids, route_weights, expert_gate, expert_up, expert_down,
    shared_gate, shared_up, shared_down,
):
    ep_count = lax.axis_size("ep")
    tp_count = lax.axis_size("tp")
    minor = 1 << (ep_count.bit_length() - 1) // 2
    rows, width = tokens.shape
    quarter = width // tp_count
    split = quarter * 3 // 4 // LANES * LANES
    expert_count = ep_count * tp_count // 2
    wide = quarter + quarter - split
    expert_iota = jnp.arange(expert_count, dtype=jnp.int32)
    table = jnp.sum(
        jnp.where(
            expert_ids[None, :, :] == expert_iota[:, None, None], route_weights[None, :, :], 0.0
        ),
        axis=2,
    )
    ff = expert_gate.shape[2]
    share = shared_gate.shape[1]
    bf16, f32 = jnp.bfloat16, jnp.float32
    dma = pltpu.SemaphoreType.DMA
    vmem = pl.BlockSpec(memory_space=pltpu.VMEM)
    anywhere = pl.BlockSpec(memory_space=pl.ANY)
    n = ep_count
    major = n // minor
    return pl.pallas_call(
        functools.partial(dense_kernel, ep_count, tp_count, minor, split),
        out_shape=jax.ShapeDtypeStruct((rows, quarter), bf16),
        in_specs=[vmem] * 3 + [anywhere] * 6,
        out_specs=vmem,
        scratch_shapes=[
            pltpu.VMEM((n, tp_count, rows, quarter), bf16),
            pltpu.VMEM((n, tp_count, rows, quarter), bf16),
            pltpu.VMEM((n, 2, rows, quarter), bf16),
            pltpu.VMEM((n, rows, split), bf16),
            pltpu.VMEM((n, rows, split), bf16),
            pltpu.VMEM((major, rows, split), bf16),
            pltpu.VMEM((major, rows, split), bf16),
            pltpu.VMEM((major, rows, split), bf16),
            pltpu.VMEM((2, major, rows, split), bf16),
            pltpu.VMEM((n, rows, wide - split), bf16),
            pltpu.VMEM((2, n, rows, wide - split), bf16),
            pltpu.VMEM((rows, wide - split), bf16),
            pltpu.VMEM((rows, wide - split), bf16),
            pltpu.VMEM((rows, quarter - split), bf16),
            pltpu.VMEM((rows, quarter - split), bf16),
            pltpu.VMEM((rows, wide), f32),
            pltpu.VMEM((n, expert_count, rows), f32),
            pltpu.VMEM((tp_count, rows, share), bf16),
            pltpu.VMEM((rows, quarter), f32),
            pltpu.VMEM((width, ff), bf16),
            pltpu.VMEM((width, ff), bf16),
            pltpu.VMEM((ff, width), bf16),
            pltpu.VMEM((width, share), bf16),
            pltpu.VMEM((width, share), bf16),
            pltpu.VMEM((share * tp_count, quarter), bf16),
            dma((6,)), dma((n,)), dma((n,)), dma((tp_count,)), dma((tp_count,)),
            dma((n, 3)), dma((n, 3)), dma((n, 3)), dma((n, 3)),
            dma((n,)), dma((n,)), dma((n, 4)), dma((n, 4)), dma((n,)), dma((n,)),
            dma((n, 2)), dma((n, 2)), dma((n,)), dma((n,)), dma((major,)), dma((major,)),
            dma((major,)), dma((2, major)), dma((n,)), dma((2, n)), dma, dma, dma, dma,
        ],
        compiler_params=pltpu.CompilerParams(
            collective_id=0, has_side_effects=True, vmem_limit_bytes=60 << 20
        ),
        name="dense_moe",
    )(
        tokens, norm_gain.reshape(1, width), table, expert_gate[0], expert_up[0], expert_down[0],
        shared_gate, shared_up, shared_down,
    )


def local(tokens, *rest):
    ep_count = lax.axis_size("ep")
    pair_count = lax.axis_size("tp") // 2
    dense_bytes = 4 * ep_count * tokens.size * tokens.dtype.itemsize
    minor = 1 << (ep_count.bit_length() - 1) // 2
    if pair_count == 2 and minor == 2 and dense_bytes <= 24 << 20:
        return dense_exchange(tokens, *rest)
    return routed_exchange(tokens, *rest)


def solution(mesh):
    return jax.shard_map(
        local,
        mesh=mesh,
        in_specs=(
            P("ep", None),
            P(),
            P("ep", None),
            P("ep", None),
            P(("ep", "tp"), None, None),
            P(("ep", "tp"), None, None),
            P(("ep", "tp"), None, None),
            P(None, "tp"),
            P(None, "tp"),
            P(None, "tp"),
        ),
        out_specs=P("ep", "tp"),
        check_vma=False,
    )
```

```python
import functools

import jax
import jax.numpy as jnp
from jax import lax
from jax.experimental import pallas as pl
from jax.experimental.pallas import tpu as pltpu
from jax.sharding import PartitionSpec as P

NORM_EPSILON = 1e-06


def swapped(block, axis, distance):
    count = lax.axis_size(axis)
    route = []
    for low in range(count):
        high = low | 1 << distance
        if high != low and high < count:
            route += [(low, high), (high, low)]
    return lax.ppermute(block, axis, route)


def routed_exchange(
    tokens,
    norm_gain,
    expert_ids,
    route_weights,
    expert_gate,
    expert_up,
    expert_down,
    shared_gate,
    shared_up,
    shared_down,
):
    ep_count = lax.axis_size("ep")
    tp_count = lax.axis_size("tp")
    pair_count = tp_count // 2
    tp_index = lax.axis_index("tp")
    column = tp_index // 2
    half_index = tp_index % 2
    token_count, model_width = tokens.shape
    top_count = expert_ids.shape[1]
    expert_count = ep_count * pair_count
    capacity = 2 * max(1, token_count * top_count // expert_count)
    half_cap = capacity // 2
    as_float = tokens.astype(jnp.float32)
    inverse_rms = lax.rsqrt(jnp.mean(as_float * as_float, axis=-1, keepdims=True) + NORM_EPSILON)
    normed = (as_float * inverse_rms * norm_gain).astype(jnp.bfloat16)
    expert_iota = jnp.arange(expert_count, dtype=jnp.int32)
    token_iota = jnp.arange(token_count, dtype=jnp.int32)
    counts = jnp.sum(
        (expert_ids[:, :, None] == expert_iota[None, None, :]).astype(jnp.bfloat16), axis=1
    )
    strict_lower = (token_iota[:, None] > token_iota[None, :]).astype(jnp.bfloat16)
    prefix = jnp.dot(strict_lower, counts, preferred_element_type=jnp.float32)
    slot_index = jnp.take_along_axis(prefix, expert_ids, axis=1).astype(jnp.int32)
    target = expert_ids // pair_count
    owner_column = expert_ids % pair_count
    is_mine = owner_column == column
    position = target * capacity + slot_index
    slot_iota = jnp.arange(ep_count * capacity, dtype=jnp.int32)
    matches = is_mine[None, :, :] & (position[None, :, :] == slot_iota[:, None, None])
    slot_taken = jnp.any(matches, axis=2)
    token_of_slot = jnp.sum(jnp.where(slot_taken, token_iota[None, :], 0), axis=1)
    filled = jnp.any(slot_taken, axis=1)
    buffer = jnp.where(
        filled[:, None], jnp.take(normed, token_of_slot, axis=0), jnp.zeros((), jnp.bfloat16)
    )
    buffer = buffer.reshape(ep_count, capacity, model_width)
    gate_local = expert_gate[0]
    up_local = expert_up[0]
    down_local = expert_down[0]
    received = lax.all_to_all(buffer, "ep", split_axis=0, concat_axis=0, tiled=True)
    flat_rows = received.reshape(-1, model_width)
    hidden = (
        jax.nn.silu(jnp.dot(flat_rows, gate_local, preferred_element_type=jnp.float32))
        * jnp.dot(flat_rows, up_local, preferred_element_type=jnp.float32)
    ).astype(jnp.bfloat16)
    partial_out = jnp.dot(hidden, down_local, preferred_element_type=jnp.float32).astype(
        jnp.bfloat16
    )
    partial_out = partial_out.reshape(received.shape[0], received.shape[1], model_width)
    kept_part = lax.dynamic_slice_in_dim(partial_out, half_index * half_cap, half_cap, 1)
    other_part = lax.dynamic_slice_in_dim(partial_out, (1 - half_index) * half_cap, half_cap, 1)
    partner_part = swapped(other_part, "tp", 0)
    expert_out = (kept_part.astype(jnp.float32) + partner_part.astype(jnp.float32)).astype(
        jnp.bfloat16
    )
    returned = lax.all_to_all(expert_out, "ep", split_axis=0, concat_axis=0, tiled=True)
    row_total = ep_count * half_cap
    flat_rows = returned.reshape(row_total, model_width).astype(jnp.float32)
    is_valid = is_mine & (slot_index // half_cap == half_index)
    row_index = jnp.where(is_valid, target * half_cap + slot_index % half_cap, -1)
    row_iota = jnp.arange(row_total, dtype=jnp.int32)
    hits = row_index[:, :, None] == row_iota[None, None, :]
    combine_table = jnp.sum(jnp.where(hits, route_weights[:, :, None], 0.0), axis=1)
    partial_routed = jnp.dot(
        combine_table,
        flat_rows,
        precision=lax.Precision.HIGHEST,
        preferred_element_type=jnp.float32,
    )
    routed = lax.psum_scatter(partial_routed, "tp", scatter_dimension=1, tiled=True)
    shared_act = (
        jax.nn.silu(jnp.dot(normed, shared_gate, preferred_element_type=jnp.float32))
        * jnp.dot(normed, shared_up, preferred_element_type=jnp.float32)
    ).astype(jnp.bfloat16)
    shared_out = jnp.dot(
        lax.all_gather(shared_act, "tp", axis=1, tiled=True),
        shared_down,
        preferred_element_type=jnp.float32,
    )
    return (routed + shared_out).astype(jnp.bfloat16)


MESH = pl.DeviceIdType.MESH
LANES = 128


def silu(v):
    return v / (1.0 + jnp.exp(-v))


def dense_kernel(
    ep_count, tp_count, minor, split,
    tok_ref, gain_ref, wt_ref, gate_hbm, up_hbm, down_hbm, sg_hbm, su_hbm, sd_hbm,
    out_ref,
    x_buf, y_buf, c_buf, xs_buf, xr_buf, ysa_buf, yra_buf, zsa_buf, zra_buf, zs_buf, zr_buf,
    ys_buf, yr_buf, fs_buf, fr_buf,
    acc, wt_all, sh_all, sh_out, gate, up, down, sg, su, sd,
    load_sem, wt_s, wt_r, sh_s, sh_r, y_s, u_s, d_s, z_r, x_s, x_r, c_s, c_r,
    ya_s, ya_r, yc_s, yc_r, rx_s, rx_r, rya_s, rya_r, rza_s, rza_r, rz_s, rz_r, ry_s, ry_r,
    f_s, f_r,
):
    major = ep_count // minor
    rows = tok_ref.shape[0]
    quarter = x_buf.shape[3]
    e = lax.axis_index("ep")
    t = lax.axis_index("tp")
    z = e // minor
    y = e % minor
    xi = t // 2
    c = t % 2
    t2 = 2 * (1 - xi) + c
    mate_x = {"tp": t2}
    mate_c = {"tp": 2 * xi + 1 - c}
    mate_y = {"ep": z * minor + 1 - y}
    z_up = {"ep": lax.rem(e + minor, ep_count)}
    z_down = {"ep": lax.rem(e + ep_count - minor, ep_count)}
    head_cols = pl.ds(0, split)
    rest_cols = pl.ds(split, quarter - split)

    def remote(src, dst, s, r, who):
        return pltpu.make_async_remote_copy(
            src_ref=src, dst_ref=dst, send_sem=s, recv_sem=r, device_id=who, device_id_type=MESH
        )

    loads = [
        pltpu.make_async_copy(a, b, load_sem.at[i])
        for i, (a, b) in enumerate(
            ((sg_hbm, sg), (su_hbm, su), (gate_hbm, gate), (up_hbm, up), (down_hbm, down), (sd_hbm, sd))
        )
    ]
    for load in loads:
        load.start()

    barrier = pltpu.get_barrier_semaphore()
    for k in range(1, ep_count):
        pl.semaphore_signal(barrier, inc=1, device_id={"ep": lax.rem(e + k, ep_count)}, device_id_type=MESH)
    for k in range(1, tp_count):
        pl.semaphore_signal(barrier, inc=1, device_id={"tp": lax.rem(t + k, tp_count)}, device_id_type=MESH)

    step = 16

    def norm_rows(i, carry):
        part = pl.ds(pl.multiple_of(i * step, step), step)
        v = tok_ref[part, :].astype(jnp.float32)
        r = lax.rsqrt(jnp.mean(v * v, axis=-1, keepdims=True) + NORM_EPSILON)
        n = (v * r * gain_ref[...]).astype(jnp.bfloat16)
        for q in range(tp_count):
            x_buf[e, q, part, :] = n[:, q * quarter : (q + 1) * quarter]
        return carry

    lax.fori_loop(0, rows // step, norm_rows, 0)
    pl.semaphore_wait(barrier, ep_count + tp_count - 2)

    def wt_copy(k, slot, who):
        src = wt_ref if slot is None else wt_all.at[slot]
        dst = wt_all.at[e if slot is None else slot]
        return remote(src, dst, wt_s.at[k], wt_r.at[k], {"ep": who})

    def head_of(g, q):
        return x_buf.at[g, q, :, head_cols]

    def rest_of(g, q):
        return x_buf.at[g, q, :, rest_cols]

    def line_head(g, s, who):
        return (remote(head_of(g, t), head_of(g, t), s.at[g, 0], z_r.at[g, 0], who),)

    def line_rest(g, s, who):
        return (
            remote(rest_of(g, t), rest_of(g, t), s.at[g, 1], z_r.at[g, 1], who),
            remote(rest_of(g, t2), rest_of(g, t2), s.at[g, 2], z_r.at[g, 2], who),
        )

    def y_copy_head(g):
        return remote(head_of(g, t), head_of(g, t), ya_s.at[g], ya_r.at[g], mate_y)

    def x_copy(g):
        ref = x_buf.at[g, t, :, head_cols]
        return remote(ref, ref, x_s.at[g], x_r.at[g], mate_x)

    def x_arrival(g):
        ref = x_buf.at[g, t2, :, head_cols]
        return remote(ref, ref, x_s.at[g], x_r.at[g], mate_x)

    def c_copies(g, lane):
        main, other = 2 * xi + lane, 2 * (1 - xi) + lane
        refs = (head_of(g, main), rest_of(g, main), rest_of(g, other), head_of(g, other))
        return [remote(r, r, c_s.at[g, i], c_r.at[g, i], mate_c) for i, r in enumerate(refs)]

    def order(j):
        k = jnp.minimum(z, major - 1 - z)
        d = (j + 1) // 2
        near = jnp.where(j % 2 == 1, z - d, z + d)
        far = jnp.where(z <= major - 1 - z, j, major - 1 - j)
        return jnp.where(j <= 2 * k, near, far)

    def slot_group(i):
        p = order(i // 2)
        yy = jnp.where(i % 2 == 0, y, 1 - y)
        return p, p * minor + yy

    def forward(p, g, pieces):
        @pl.when((p <= z) & (z < major - 1))
        def _():
            for copy in pieces(g, u_s, z_up):
                copy.start()

        @pl.when((p >= z) & (z > 0))
        def _():
            for copy in pieces(g, d_s, z_down):
                copy.start()

    for copy in line_rest(e, y_s, mate_y):
        copy.start()
    forward(z, e, line_head)
    y_copy_head(e).start()
    for k in range(1, ep_count):
        wt_copy(k, None, lax.rem(e + k, ep_count)).start()
    wt_all[e] = wt_ref[...]
    forward(z, e, line_rest)

    loads[0].wait()
    loads[1].wait()
    sg_sum = jnp.zeros((rows, sg.shape[1]), jnp.float32)
    su_sum = jnp.zeros((rows, sg.shape[1]), jnp.float32)
    for q in range(tp_count):
        band = pl.ds(q * quarter, quarter)
        sg_sum += jnp.dot(x_buf[e, q], sg[band, :], preferred_element_type=jnp.float32)
        su_sum += jnp.dot(x_buf[e, q], su[band, :], preferred_element_type=jnp.float32)
    sh_all[t] = (silu(sg_sum) * su_sum).astype(jnp.bfloat16)

    def sh_copy(k, slot, who):
        return remote(sh_all.at[slot], sh_all.at[slot], sh_s.at[k], sh_r.at[k], {"tp": who})

    for k in range(1, tp_count):
        sh_copy(k, t, lax.rem(t + k, tp_count)).start()
    for load in loads[2:5]:
        load.wait()
    for k in range(1, ep_count):
        wt_copy(k, lax.rem(e + ep_count - k, ep_count), e).wait_recv()

    expert = e * (tp_count // 2) + xi
    expert_mask = lax.broadcasted_iota(jnp.int32, wt_ref.shape, 0) == expert
    eye = lax.broadcasted_iota(jnp.int32, (rows, rows), 0) == lax.broadcasted_iota(
        jnp.int32, (rows, rows), 1
    )

    def compute(g):
        row = jnp.sum(jnp.where(expert_mask, wt_all[g], 0.0), axis=0, keepdims=True)
        weight = jnp.sum(jnp.where(eye, row, 0.0), axis=1, keepdims=True)
        ff = gate.shape[1]
        g_sum = jnp.zeros((rows, ff), jnp.float32)
        u_sum = jnp.zeros((rows, ff), jnp.float32)
        for q in range(tp_count):
            band = pl.ds(q * quarter, quarter)
            g_sum += jnp.dot(x_buf[g, q], gate[band, :], preferred_element_type=jnp.float32)
            u_sum += jnp.dot(x_buf[g, q], up[band, :], preferred_element_type=jnp.float32)
        act = (silu(g_sum) * u_sum).astype(jnp.bfloat16)
        for q in range(tp_count):
            part = jnp.dot(
                act, down[:, q * quarter : (q + 1) * quarter], preferred_element_type=jnp.float32
            )
            y_buf[g, q] = (part * weight).astype(jnp.bfloat16)

    def yc_copy(g, k):
        return remote(
            y_buf.at[g, 2 * k + 1 - c], c_buf.at[g, k], yc_s.at[g, k], yc_r.at[g, k], mate_c
        )

    def rx_copy(g):
        return remote(xs_buf.at[g], xr_buf.at[g], rx_s.at[g], rx_r.at[g], mate_x)

    def rya_copy(p):
        return remote(ysa_buf.at[p], yra_buf.at[p], rya_s.at[p], rya_r.at[p], mate_y)

    total = ep_count

    def head_sum(g):
        return (
            y_buf[g, t, :, head_cols].astype(jnp.float32)
            + c_buf[g, xi, :, head_cols].astype(jnp.float32)
            + xr_buf[g].astype(jnp.float32)
        )

    def main_step(i, carry):
        @pl.when((i >= 1) & (i < total))
        def _():
            p, g = slot_group(i)
            ours = c_copies(g, c)

            @pl.when(i % 2 == 0)
            def _():
                line_head(g, u_s, z_up)[0].wait_recv()
                forward(p, g, line_head)
                y_copy_head(g).start()
                x_copy(g).start()
                ours[0].start()

            for copy in line_rest(g, u_s, z_up):
                copy.wait_recv()
            forward(p, g, line_rest)
            ours[1].start()
            ours[2].start()

        @pl.when((i >= 2) & (i <= total) & (i % 2 == 0))
        def _():
            _, g = slot_group(i - 1)
            y_copy_head(g).wait_recv()
            x_copy(g).start()
            c_copies(g, c)[0].start()

        @pl.when((i >= 4) & (i <= total + 2))
        def _():
            _, g = slot_group(i - 3)
            x_arrival(g).wait_recv()
            c_copies(g, c)[3].start()

        @pl.when((i >= 4) & (i <= total + 3))
        def _():
            _, g = slot_group(i - 4)

            @pl.when(i >= 5)
            def _():
                for copy in c_copies(g, 1 - c):
                    copy.wait_recv()

            compute(g)
            for k in range(2):
                yc_copy(g, k).start()

        @pl.when((i >= 5) & (i <= total + 4))
        def _():
            _, g = slot_group(i - 5)
            for k in range(2):
                yc_copy(g, k).wait_recv()
            xs_buf[g] = (
                y_buf[g, t2, :, head_cols].astype(jnp.float32)
                + c_buf[g, 1 - xi, :, head_cols].astype(jnp.float32)
            ).astype(jnp.bfloat16)
            rx_copy(g).start()

        @pl.when((i >= 8) & (i % 2 == 0))
        def _():
            p, g = slot_group(i - 7)
            rx_copy(g).wait_recv()
            ysa_buf[p] = head_sum(g).astype(jnp.bfloat16)
            rya_copy(p).start()

        return carry

    lax.fori_loop(0, total + 7, main_step, 0)

    loads[5].wait()
    for k in range(1, tp_count):
        sh_copy(k, lax.rem(t + tp_count - k, tp_count), t).wait_recv()
    shared = jnp.zeros((rows, quarter), jnp.float32)
    width = sg.shape[1]
    for q in range(tp_count):
        shared += jnp.dot(
            sh_all[q], sd[q * width : (q + 1) * width, :], preferred_element_type=jnp.float32
        )
    sh_out[...] = shared

    def rz_copy(g, lane, who):
        return remote(zs_buf.at[g], zr_buf.at[lane, g], rz_s.at[g], rz_r.at[lane, g], who)

    def rza_copy(p, lane, who):
        return remote(zsa_buf.at[p], zra_buf.at[lane, p], rza_s.at[p], rza_r.at[lane, p], who)

    def sum_rest(p, g):
        acc[:, split:quarter] = y_buf[g, t, :, rest_cols].astype(jnp.float32) + c_buf[
            g, xi, :, rest_cols
        ].astype(jnp.float32)
        acc[:, quarter:] = y_buf[g, t2, :, rest_cols].astype(jnp.float32) + c_buf[
            g, 1 - xi, :, rest_cols
        ].astype(jnp.float32)

        @pl.when((p >= z) & (z > 0))
        def _():
            rz_copy(g, 0, z_up).wait_recv()
            acc[:, split:] += zr_buf[0, g].astype(jnp.float32)

        @pl.when((p <= z) & (z < major - 1))
        def _():
            rz_copy(g, 1, z_up).wait_recv()
            acc[:, split:] += zr_buf[1, g].astype(jnp.float32)

    def sum_head(p, g):
        rx_copy(g).wait_recv()
        rya_copy(p).wait_recv()
        acc[:, :split] = head_sum(g) + yra_buf[p].astype(jnp.float32)

        @pl.when((p >= z) & (z > 0))
        def _():
            rza_copy(p, 0, z_up).wait_recv()
            acc[:, :split] += zra_buf[0, p].astype(jnp.float32)

        @pl.when((p <= z) & (z < major - 1))
        def _():
            rza_copy(p, 1, z_up).wait_recv()
            acc[:, :split] += zra_buf[1, p].astype(jnp.float32)

    def sum_step(q, carry):
        ups = major - 1 - z
        low = jnp.where(q < ups, z + 1 + q, z - 1 - (q - ups))
        high = jnp.where(q < z, z - 1 - q, z + 1 + (q - z))
        p = jnp.where(2 * z < major, low, high)

        def send(copy, key):
            @pl.when(p > z)
            def _():
                copy(key, 0, z_up).start()

            @pl.when(p < z)
            def _():
                copy(key, 1, z_down).start()

        for yy in (1 - y, y):
            g = p * minor + yy
            sum_rest(p, g)
            zs_buf[g] = acc[:, split:].astype(jnp.bfloat16)
            send(rz_copy, g)
        sum_head(p, p * minor + y)
        zsa_buf[p] = acc[:, :split].astype(jnp.bfloat16)
        send(rza_copy, p)
        return carry

    lax.fori_loop(0, major - 1, sum_step, 0)

    y_copy = remote(ys_buf, yr_buf, ry_s, ry_r, mate_y)
    sum_rest(z, z * minor + 1 - y)
    ys_buf[...] = acc[:, split:].astype(jnp.bfloat16)
    y_copy.start()
    sum_rest(z, e)
    sum_head(z, e)
    y_copy.wait_recv()
    acc[:, split:] += yr_buf[...].astype(jnp.float32)
    final = acc[...]
    f_copy = remote(fs_buf, fr_buf, f_s, f_r, mate_x)
    fs_buf[...] = final[:, quarter:].astype(jnp.bfloat16)
    f_copy.start()
    out_ref[:, :split] = (final[:, :split] + sh_out[:, :split]).astype(jnp.bfloat16)
    f_copy.wait_recv()
    out_ref[:, split:] = (
        final[:, split:quarter] + fr_buf[...].astype(jnp.float32) + sh_out[:, split:]
    ).astype(jnp.bfloat16)

    f_copy.wait_send()
    y_copy.wait_send()
    for copy in line_rest(e, y_s, mate_y):
        copy.wait_send()
    for k in range(1, ep_count):
        wt_copy(k, None, lax.rem(e + k, ep_count)).wait_send()
    for k in range(1, tp_count):
        sh_copy(k, t, lax.rem(t + k, tp_count)).wait_send()

    def drain(i, carry):
        p, g = slot_group(i)

        def sent(pieces):
            @pl.when((p <= z) & (z < major - 1))
            def _():
                for copy in pieces(g, u_s, z_up):
                    copy.wait_send()

            @pl.when((p >= z) & (z > 0))
            def _():
                for copy in pieces(g, d_s, z_down):
                    copy.wait_send()

        sent(line_rest)

        @pl.when(i % 2 == 0)
        def _():
            sent(line_head)
            y_copy_head(g).wait_send()

            @pl.when(p != z)
            def _():
                rza_copy(p, 0, z_up).wait_send()

        @pl.when(i % 2 == 1)
        def _():
            rya_copy(p).wait_send()

        @pl.when(i > 0)
        def _():
            x_copy(g).wait_send()
            for copy in c_copies(g, c):
                copy.wait_send()

        for k in range(2):
            yc_copy(g, k).wait_send()
        rx_copy(g).wait_send()

        @pl.when(p != z)
        def _():
            rz_copy(g, 0, z_up).wait_send()

        return carry

    lax.fori_loop(0, total, drain, 0)


def dense_exchange(
    tokens, norm_gain, expert_ids, route_weights, expert_gate, expert_up, expert_down,
    shared_gate, shared_up, shared_down,
):
    ep_count = lax.axis_size("ep")
    tp_count = lax.axis_size("tp")
    minor = 1 << (ep_count.bit_length() - 1) // 2
    rows, width = tokens.shape
    quarter = width // tp_count
    split = quarter * 3 // 4 // LANES * LANES
    expert_count = ep_count * tp_count // 2
    wide = quarter + quarter - split
    expert_iota = jnp.arange(expert_count, dtype=jnp.int32)
    table = jnp.sum(
        jnp.where(
            expert_ids[None, :, :] == expert_iota[:, None, None], route_weights[None, :, :], 0.0
        ),
        axis=2,
    )
    ff = expert_gate.shape[2]
    share = shared_gate.shape[1]
    bf16, f32 = jnp.bfloat16, jnp.float32
    dma = pltpu.SemaphoreType.DMA
    vmem = pl.BlockSpec(memory_space=pltpu.VMEM)
    anywhere = pl.BlockSpec(memory_space=pl.ANY)
    n = ep_count
    major = n // minor
    return pl.pallas_call(
        functools.partial(dense_kernel, ep_count, tp_count, minor, split),
        out_shape=jax.ShapeDtypeStruct((rows, quarter), bf16),
        in_specs=[vmem] * 3 + [anywhere] * 6,
        out_specs=vmem,
        scratch_shapes=[
            pltpu.VMEM((n, tp_count, rows, quarter), bf16),
            pltpu.VMEM((n, tp_count, rows, quarter), bf16),
            pltpu.VMEM((n, 2, rows, quarter), bf16),
            pltpu.VMEM((n, rows, split), bf16),
            pltpu.VMEM((n, rows, split), bf16),
            pltpu.VMEM((major, rows, split), bf16),
            pltpu.VMEM((major, rows, split), bf16),
            pltpu.VMEM((major, rows, split), bf16),
            pltpu.VMEM((2, major, rows, split), bf16),
            pltpu.VMEM((n, rows, wide - split), bf16),
            pltpu.VMEM((2, n, rows, wide - split), bf16),
            pltpu.VMEM((rows, wide - split), bf16),
            pltpu.VMEM((rows, wide - split), bf16),
            pltpu.VMEM((rows, quarter - split), bf16),
            pltpu.VMEM((rows, quarter - split), bf16),
            pltpu.VMEM((rows, wide), f32),
            pltpu.VMEM((n, expert_count, rows), f32),
            pltpu.VMEM((tp_count, rows, share), bf16),
            pltpu.VMEM((rows, quarter), f32),
            pltpu.VMEM((width, ff), bf16),
            pltpu.VMEM((width, ff), bf16),
            pltpu.VMEM((ff, width), bf16),
            pltpu.VMEM((width, share), bf16),
            pltpu.VMEM((width, share), bf16),
            pltpu.VMEM((share * tp_count, quarter), bf16),
            dma((6,)), dma((n,)), dma((n,)), dma((tp_count,)), dma((tp_count,)),
            dma((n, 3)), dma((n, 3)), dma((n, 3)), dma((n, 3)),
            dma((n,)), dma((n,)), dma((n, 4)), dma((n, 4)), dma((n,)), dma((n,)),
            dma((n, 2)), dma((n, 2)), dma((n,)), dma((n,)), dma((major,)), dma((major,)),
            dma((major,)), dma((2, major)), dma((n,)), dma((2, n)), dma, dma, dma, dma,
        ],
        compiler_params=pltpu.CompilerParams(
            collective_id=0, has_side_effects=True, vmem_limit_bytes=60 << 20
        ),
        name="dense_moe",
    )(
        tokens, norm_gain.reshape(1, width), table, expert_gate[0], expert_up[0], expert_down[0],
        shared_gate, shared_up, shared_down,
    )


def local(tokens, *rest):
    ep_count = lax.axis_size("ep")
    pair_count = lax.axis_size("tp") // 2
    dense_bytes = 4 * ep_count * tokens.size * tokens.dtype.itemsize
    minor = 1 << (ep_count.bit_length() - 1) // 2
    if pair_count == 2 and minor == 2 and dense_bytes <= 24 << 20:
        return dense_exchange(tokens, *rest)
    return routed_exchange(tokens, *rest)


def solution(mesh):
    return jax.shard_map(
        local,
        mesh=mesh,
        in_specs=(
            P("ep", None),
            P(),
            P("ep", None),
            P("ep", None),
            P(("ep", "tp"), None, None),
            P(("ep", "tp"), None, None),
            P(("ep", "tp"), None, None),
            P(None, "tp"),
            P(None, "tp"),
            P(None, "tp"),
        ),
        out_specs=P("ep", "tp"),
        check_vma=False,
    )
```
